32 devices in a mesh: sp: 16 (over z, y, x), tp: 2 (over core).
Axes of the slice: x: 2, y: 2, z: 4, core: 2. Of those that a mesh axis runs over, the one named last changes fastest.
Arguments:
- target: bfloat16 [4096, 1024], P(('sp', 'tp')), may hold values from -60 to 60
- source: bfloat16 [2048, 1024], P('sp'), may hold values from -7 to 7
- target_gains: bfloat16 [2, 4, 1024], replicated, may hold values from 0.099609375 to 1.8984375
- source_gain: bfloat16 [2, 1024], replicated, may hold values from 0.099609375 to 1.8984375
- query_weight: bfloat16 [2, 1024, 1024], P(None, None, 'tp'), may hold values from -0.1875 to 0.1875
- key_weight: bfloat16 [2, 1024, 1024], P(None, None, 'tp'), may hold values from -7.5625 to 7.5625
- value_weight: bfloat16 [2, 1024, 1024], P(None, None, 'tp'), may hold values from -0.1875 to 0.1875
- out_weight: bfloat16 [2, 1024, 1024], P(None, 'tp'), may hold values from -0.1875 to 0.1875
- gate_weight: bfloat16 [2, 1024, 1536], P(None, None, 'tp'), may hold values from -0.1875 to 0.1875
- up_weight: bfloat16 [2, 1024, 1536], P(None, None, 'tp'), may hold values from -0.1875 to 0.1875
- down_weight: bfloat16 [2, 1536, 1024], P(None, 'tp'), may hold values from -0.15625 to 0.15625
Outputs:
- stream: bfloat16 [4096, 1024], P(('sp', 'tp'))
The draws below stay inside these ranges and needn't reach their ends.
All inputs are finite; a program needn't handle non-finite values.
Results may differ from the reference program's by a relative error of at most 0.04.
Values may be sent and summed in bfloat16 or wider, within the bound.
A program may use at most 64 MiB of HBM per device.

```python
import jax
import jax.numpy as jnp
from jax import lax

D = 1024
HEADS = 8
HEAD_DIM = 128
FF = 1536
LAYERS = 2
TGT_DEV = 256
TGT = 4096
SRC = 2048
N_TP = 2


def drawn_rows(key):
    base = jnp.clip(jax.random.normal(jax.random.fold_in(key, 101), (TGT, D), jnp.float32), -6.0, 6.0)
    return base


def draw_target(key, part):
    base = drawn_rows(key)
    return base.astype(jnp.bfloat16)


def draw_source(key, part):
    noise = jnp.clip(jax.random.normal(jax.random.fold_in(key, 105), (SRC, D), jnp.float32), -6.0, 6.0)
    return noise.astype(jnp.bfloat16)


def head_weights(key):
    shape = (LAYERS, D, HEADS * HEAD_DIM)
    first = jnp.clip(jax.random.normal(jax.random.fold_in(key, 201), shape, jnp.float32), -6.0, 6.0) * D ** (-0.5)
    second = jnp.clip(jax.random.normal(jax.random.fold_in(key, 202), shape, jnp.float32), -6.0, 6.0) * D ** (-0.5)
    return (first, second)


def draw_query_weight(key, part):
    first, second = head_weights(key)
    return first.astype(jnp.bfloat16)


def draw_key_weight(key, part):
    first, second = head_weights(key)
    return second.astype(jnp.bfloat16)


def block_scale(stream_key, dims, pieces, smallest, largest):
    loudness = 1.0
    for axis_at, parts in pieces:
        heights = jax.random.uniform(jax.random.fold_in(jax.random.fold_in(stream_key, 6), axis_at), (parts,), jnp.float32, smallest / len(pieces), largest / len(pieces))
        loudness = loudness * jnp.repeat(jnp.exp(heights), dims[axis_at] // parts).reshape((-1,) + (1,) * (len(dims) - 1 - axis_at))
    return loudness


def gaussian(rng, shape, spread, most, pieces=(), kind=jnp.bfloat16):
    values = jax.random.normal(rng, shape, jnp.float32) * spread
    if len(pieces) > 0:
        values = block_scale(rng, shape, pieces, -0.22, 0.18) * values
    return jnp.clip(values, min=-most, max=most).astype(kind)


def setup_inputs(seed: int = 0) -> dict:
    key_list = jax.random.split(jax.random.key(seed), 12)
    target = draw_target(jax.random.fold_in(key_list[11], 71), 0)
    source = draw_source(jax.random.fold_in(key_list[11], 71), 0)
    target_gains = jnp.clip(1.0 + 0.18 * jax.random.normal(key_list[2], (LAYERS, 4, D), jnp.float32), 0.099609375, 1.8984375).astype(jnp.bfloat16)
    source_gain = jnp.clip(1.0 + 0.18 * jax.random.normal(key_list[3], (LAYERS, D), jnp.float32), 0.099609375, 1.8984375).astype(jnp.bfloat16)
    query_weight = draw_query_weight(jax.random.fold_in(key_list[11], 71), 0)
    key_weight = draw_key_weight(jax.random.fold_in(key_list[11], 71), 0)
    value_weight = gaussian(key_list[6], (LAYERS, D, HEADS * HEAD_DIM), D ** -0.5, 0.1875, ((2, 2),))
    out_weight = gaussian(key_list[7], (LAYERS, HEADS * HEAD_DIM, D), (HEADS * HEAD_DIM) ** -0.5, 0.1875, ((1, 2),))
    gate_weight = gaussian(key_list[8], (LAYERS, D, FF), D ** -0.5, 0.1875, ((2, 2),))
    up_weight = gaussian(key_list[9], (LAYERS, D, FF), D ** -0.5, 0.1875, ((2, 2),))
    down_weight = gaussian(key_list[10], (LAYERS, FF, D), FF ** -0.5, 0.15625, ((1, 2),))
    return dict(target=target, source=source, target_gains=target_gains, source_gain=source_gain, query_weight=query_weight, key_weight=key_weight, value_weight=value_weight, out_weight=out_weight, gate_weight=gate_weight, up_weight=up_weight, down_weight=down_weight)


epsilon = 1e-06

def rms_norm(values, gain_row):
    widened = values.astype(jnp.float32)
    inverse = lax.rsqrt(lax.optimization_barrier(jnp.mean(widened * widened, axis=-1, keepdims=True)) + epsilon)
    return widened * inverse * gain_row.astype(jnp.float32)

def blockwise_sum(left, right, pieces_count):
    block_width = left.shape[1] // pieces_count
    summed = jnp.zeros((left.shape[0], right.shape[1]), jnp.float32)
    for index in range(pieces_count):
        partial_value = jnp.dot(left[:, index * block_width:(index + 1) * block_width], right[index * block_width:(index + 1) * block_width], preferred_element_type=jnp.float32)
        summed = summed + lax.optimization_barrier(partial_value.astype(jnp.bfloat16)).astype(jnp.float32)
    return summed.astype(jnp.bfloat16)

def reference(target, source, target_gains, source_gain, query_weight, key_weight, value_weight, out_weight, gate_weight, up_weight, down_weight):
    factor = HEAD_DIM ** (-0.5)
    stream = target
    for layer_index in range(LAYERS):
        layer_gains = target_gains[layer_index]
        normed_source = rms_norm(source, source_gain[layer_index]).astype(jnp.bfloat16)
        key_rows = jnp.dot(normed_source, key_weight[layer_index], preferred_element_type=jnp.float32).astype(jnp.bfloat16)
        value_rows = jnp.dot(normed_source, value_weight[layer_index], preferred_element_type=jnp.float32).astype(jnp.bfloat16)
        key_wide = key_rows.astype(jnp.float32).reshape(SRC, HEADS, HEAD_DIM)
        value_wide = value_rows.astype(jnp.float32).reshape(SRC, HEADS, HEAD_DIM)
        normed = rms_norm(stream, layer_gains[0]).astype(jnp.bfloat16)
        queries = jnp.dot(normed, query_weight[layer_index], preferred_element_type=jnp.float32).astype(jnp.bfloat16)
        query_blocks = queries.astype(jnp.float32).reshape(TGT // TGT_DEV, TGT_DEV, HEADS, HEAD_DIM)

        def attend(query_block):
            scores = jnp.einsum('thd,shd->ths', query_block, key_wide) * factor
            row_max = lax.optimization_barrier(jnp.max(scores, axis=-1, keepdims=True))
            weights = jnp.exp(scores - row_max)
            totals = lax.optimization_barrier(jnp.sum(weights, axis=-1))
            rounded = lax.optimization_barrier(weights.astype(jnp.bfloat16)).astype(jnp.float32)
            blended = jnp.einsum('ths,shd->thd', rounded, value_wide)
            return (blended / totals[..., None]).astype(jnp.bfloat16)
        context = lax.map(attend, query_blocks).reshape(TGT, HEADS * HEAD_DIM)
        attended = blockwise_sum(context, out_weight[layer_index], N_TP)
        stream = (stream.astype(jnp.float32) + rms_norm(attended, layer_gains[1])).astype(jnp.bfloat16)
        mixer_in = rms_norm(stream, layer_gains[2]).astype(jnp.bfloat16)
        gate_part = jnp.dot(mixer_in, gate_weight[layer_index], preferred_element_type=jnp.float32)
        up_part = jnp.dot(mixer_in, up_weight[layer_index], preferred_element_type=jnp.float32)
        hidden = (jax.nn.silu(gate_part) * up_part).astype(jnp.bfloat16)
        mixer_out = blockwise_sum(hidden, down_weight[layer_index], N_TP)
        stream = (stream.astype(jnp.float32) + rms_norm(mixer_out, layer_gains[3])).astype(jnp.bfloat16)
    return stream
```

```python
import functools
import math

import jax
import jax.numpy as jnp
from jax import lax
from jax.experimental import pallas as pl
from jax.experimental.pallas import tpu as pltpu
from jax.sharding import PartitionSpec as P

HEAD_DIM = 128


epsilon = 1e-06


def rms_norm(values, gain_row):
    widened = values.astype(jnp.float32)
    inverse = lax.rsqrt(jnp.mean(widened * widened, axis=-1, keepdims=True) + epsilon)
    return widened * inverse * gain_row.astype(jnp.float32)


def per_device(
    target,
    source,
    target_gains,
    source_gain,
    query_weight,
    key_weight,
    value_weight,
    out_weight,
    gate_weight,
    up_weight,
    down_weight,
):
    layers = query_weight.shape[0]
    own_rows = target.shape[0]
    heads_dev = query_weight.shape[2] // HEAD_DIM
    factor = HEAD_DIM ** (-0.5)

    def source_heads(layer_index):
        normed_source = rms_norm(source, source_gain[layer_index]).astype(jnp.bfloat16)
        key_rows = jnp.dot(
            normed_source, key_weight[layer_index], preferred_element_type=jnp.float32
        ).astype(jnp.bfloat16)
        value_rows = jnp.dot(
            normed_source, value_weight[layer_index], preferred_element_type=jnp.float32
        ).astype(jnp.bfloat16)
        return (key_rows, value_rows)

    projected = [source_heads(layer_index) for layer_index in range(layers)]
    every_key = jnp.stack([entry[0] for entry in projected])
    every_value = jnp.stack([entry[1] for entry in projected])
    every_key, every_value = (
        lax.all_gather(every_key, "sp", axis=1, tiled=True),
        lax.all_gather(every_value, "sp", axis=1, tiled=True),
    )
    sp_count = lax.axis_size("sp")
    source_rows = source.shape[0]
    grouping = 1
    while grouping * 2 * source_rows <= 512 and sp_count % (grouping * 2) == 0:
        grouping = grouping * 2
    stream = target
    for layer_index in range(layers):
        layer_gains = target_gains[layer_index]
        normed = rms_norm(stream, layer_gains[0]).astype(jnp.bfloat16)

        def query_piece(row_piece, offset, layer_index=layer_index):
            return jnp.dot(
                row_piece, query_weight[layer_index], preferred_element_type=jnp.float32
            ).astype(jnp.bfloat16)

        queries = query_piece(lax.all_gather(normed, "tp", axis=0, tiled=True), jnp.int32(0))
        group_rows = queries.shape[0]
        query_heads = queries.reshape(group_rows, heads_dev, HEAD_DIM)

        def attend(folded, pieces, offset, query_heads=query_heads):
            running_max, running_sum, weighted = folded
            key_heads = pieces[0].reshape(pieces[0].shape[0], heads_dev, HEAD_DIM)
            value_heads = pieces[1].reshape(pieces[1].shape[0], heads_dev, HEAD_DIM)
            scores = (
                jnp.einsum(
                    "thd,shd->ths", query_heads, key_heads, preferred_element_type=jnp.float32
                )
                * factor
            )
            new_max = jnp.maximum(running_max, jnp.max(scores, axis=-1))
            shrink = jnp.exp(running_max - new_max)
            weights = jnp.exp(scores - new_max[..., None])
            running_sum = running_sum * shrink + jnp.sum(weights, axis=-1)
            weighted = weighted * shrink[..., None] + jnp.einsum(
                "ths,shd->thd",
                weights.astype(jnp.bfloat16),
                value_heads,
                preferred_element_type=jnp.float32,
            )
            return (new_max, running_sum, weighted)

        initial = (
            jnp.full((group_rows, heads_dev), -1e30, jnp.float32),
            jnp.zeros((group_rows, heads_dev), jnp.float32),
            jnp.zeros((group_rows, heads_dev, HEAD_DIM), jnp.float32),
        )
        columns = every_key.shape[2]
        key_blocks = every_key[layer_index].reshape(
            sp_count // grouping, grouping * source_rows, columns
        )
        value_blocks = every_value[layer_index].reshape(
            sp_count // grouping, grouping * source_rows, columns
        )

        def scan_step(carry, blocks, attend=attend):
            return (attend(carry, blocks, 0), None)

        folded, unused = lax.scan(scan_step, initial, (key_blocks, value_blocks))
        running_max, running_sum, weighted = folded
        context = (
            (weighted / running_sum[..., None])
            .reshape(group_rows, heads_dev * HEAD_DIM)
            .astype(jnp.bfloat16)
        )

        def attn_term(offset, length, layer_index=layer_index, context=context):
            return jnp.dot(context, out_weight[layer_index], preferred_element_type=jnp.float32)

        attended = lax.psum_scatter(
            attn_term(jnp.int32(0), lax.axis_size("tp") * own_rows).astype(jnp.bfloat16),
            "tp",
            scatter_dimension=0,
            tiled=True,
        )
        stream = (stream.astype(jnp.float32) + rms_norm(attended, layer_gains[1])).astype(
            jnp.bfloat16
        )
        mixer_in = rms_norm(stream, layer_gains[2]).astype(jnp.bfloat16)

        def mixer_piece(row_piece, offset, layer_index=layer_index):
            gate_part = jnp.dot(
                row_piece, gate_weight[layer_index], preferred_element_type=jnp.float32
            )
            up_part = jnp.dot(row_piece, up_weight[layer_index], preferred_element_type=jnp.float32)
            return (jax.nn.silu(gate_part) * up_part).astype(jnp.bfloat16)

        hidden = mixer_piece(lax.all_gather(mixer_in, "tp", axis=0, tiled=True), jnp.int32(0))

        def mixer_term(offset, length, layer_index=layer_index, hidden=hidden):
            return jnp.dot(hidden, down_weight[layer_index], preferred_element_type=jnp.float32)

        mixer_out = lax.psum_scatter(
            mixer_term(jnp.int32(0), lax.axis_size("tp") * own_rows).astype(jnp.bfloat16),
            "tp",
            scatter_dimension=0,
            tiled=True,
        )
        stream = (stream.astype(jnp.float32) + rms_norm(mixer_out, layer_gains[3])).astype(
            jnp.bfloat16
        )
    return stream


MESH = pl.DeviceIdType.MESH
F32 = jnp.float32
BF16 = jnp.bfloat16
KZ, KX, KY, KDX, KDY, TZ, TX, TY, TDX, TDY = range(10)


def dot(a, b):
    return jnp.dot(a, b, preferred_element_type=F32)


def fused_kernel(
    grid,
    target,
    source,
    target_gains,
    source_gain,
    wq_hbm,
    wk_hbm,
    wv_hbm,
    wo_hbm,
    wg_hbm,
    wu_hbm,
    wd_hbm,
    out_ref,
    stream,
    src,
    wq,
    wk,
    wv,
    wo,
    wg,
    wu,
    wd,
    keys,
    values,
    queries,
    maxima,
    acc,
    part,
    got,
    send,
    recv,
    xsend,
    xrecv,
    wsem,
    lsem,
):
    size_x, size_y, size_z = grid
    layers = wq.shape[0]
    own = target.shape[0]
    rows = source.shape[0]
    heads = wq.shape[2] // HEAD_DIM
    half, quarter = rows // 2, rows // 4
    chunk = 4 * rows
    sp = lax.axis_index("sp")
    core = lax.axis_index("tp")
    other = 1 - core
    x = lax.rem(sp, size_x)
    y = lax.rem(lax.div(sp, size_x), size_y)
    z = lax.div(sp, size_x * size_y)

    def at(xx, yy, zz, cc):
        return {"sp": (zz * size_y + yy) * size_x + xx, "tp": cc}

    def flip(j):
        low = lax.rem(lax.rem(z, 2) + j % 2, 2)
        high = lax.rem(lax.div(z, 2) + j // 2, 2)
        return low + 2 * high

    x_peer = at(1 - x, y, z, core)
    y_peer = at(x, 1 - y, z, core)
    tp_peer = at(x, y, z, other)
    z_peers = [at(x, y, flip(j), core) for j in range(size_z)]

    own_rows = pl.ds(pl.multiple_of(core * own, own), own)
    other_rows = pl.ds(pl.multiple_of(other * own, own), own)
    source_copy = pltpu.make_async_copy(source, src.at[0, 0], lsem.at[0])
    target_copy = pltpu.make_async_copy(target, stream.at[own_rows], lsem.at[1])
    source_copy.start()
    target_copy.start()
    pairs = [(wk_hbm, wk), (wv_hbm, wv), (wq_hbm, wq), (wo_hbm, wo), (wg_hbm, wg), (wu_hbm, wu), (wd_hbm, wd)]
    fetch = {}
    for layer in range(layers):
        for k, (a, b) in enumerate(pairs):
            fetch[k, layer] = pltpu.make_async_copy(a.at[layer], b.at[layer], wsem.at[k, layer])

    barrier = pltpu.get_barrier_semaphore()
    peers = [x_peer, y_peer, tp_peer] + z_peers[1:]
    for peer in peers:
        pl.semaphore_signal(barrier, inc=1, device_id=peer, device_id_type=MESH)
    for k in (2, 0, 1):
        fetch[k, 0].start()
    for k in (0, 1):
        for layer in range(1, layers):
            fetch[k, layer].start()
    pl.semaphore_wait(barrier, len(peers))

    def mine(c):
        return pl.ds(pl.multiple_of(c * half, half), half)

    def first(c):
        return pl.ds(pl.multiple_of(c * half, quarter), quarter)

    def second(c):
        return pl.ds(pl.multiple_of(c * half + quarter, quarter), quarter)

    def copy(kind, j, from_ref, to_ref, peer):
        return pltpu.make_async_remote_copy(
            src_ref=from_ref,
            dst_ref=to_ref,
            send_sem=send.at[kind, j],
            recv_sem=recv.at[kind, j],
            device_id=peer,
            device_id_type=MESH,
        )

    def blk(j, sub, sl):
        return src.at[j, sub, sl]

    def to_z(j):
        return copy(KZ, j, blk(0, 0, mine(core)), blk(j, 0, mine(core)), z_peers[j])

    def to_x(j):
        return copy(KX, j, blk(j, 0, mine(core)), blk(j, 1, mine(core)), x_peer)

    def to_y(j):
        return copy(KY, j, blk(j, 0, mine(core)), blk(j, 2, mine(core)), y_peer)

    def diag_y(j):
        return copy(KDY, j, blk(j, 1, first(core)), blk(j, 3, first(core)), y_peer)

    def diag_x(j):
        return copy(KDX, j, blk(j, 2, second(core)), blk(j, 3, second(core)), x_peer)

    def to_tp(kind, j, c):
        sub = {TZ: 0, TX: 1, TY: 2, TDX: 3, TDY: 3}[kind]
        sl = {TDX: second, TDY: first}.get(kind, mine)(c)
        return copy(kind, j, blk(j, sub, sl), blk(j, sub, sl), tp_peer)

    def z_arrived(zj, static):
        copy(KZ, zj, blk(zj, 0, mine(core)), blk(zj, 0, mine(core)), x_peer).wait_recv()
        to_x(zj).start()
        to_y(zj).start()
        to_tp(TZ, zj, core).start()

    def xy_arrived(j):
        copy(KX, j, blk(j, 1, mine(core)), blk(j, 1, mine(core)), x_peer).wait_recv()
        diag_y(j).start()
        to_tp(TX, j, core).start()
        copy(KY, j, blk(j, 2, mine(core)), blk(j, 2, mine(core)), y_peer).wait_recv()
        diag_x(j).start()
        to_tp(TY, j, core).start()

    def diag_arrived(j):
        copy(KDY, j, blk(j, 3, first(core)), blk(j, 3, first(core)), y_peer).wait_recv()
        to_tp(TDY, j, core).start()
        copy(KDX, j, blk(j, 3, second(core)), blk(j, 3, second(core)), x_peer).wait_recv()
        to_tp(TDX, j, core).start()

    def xcopy(e, from_ref, to_ref):
        return pltpu.make_async_remote_copy(
            src_ref=from_ref,
            dst_ref=to_ref,
            send_sem=xsend.at[e],
            recv_sem=xrecv.at[e],
            device_id=tp_peer,
            device_id_type=MESH,
        )

    source_copy.wait()
    to_x(0).start()
    to_y(0).start()
    for j in range(1, size_z):
        to_z(j).start()
    target_copy.wait()
    give = xcopy(0, stream.at[own_rows], stream.at[own_rows])
    give.start()
    for layer in range(layers):
        for k in (2, 3, 4, 5, 6):
            if (k, layer) != (2, 0):
                fetch[k, layer].start()

    def rms(v, gain):
        inverse = lax.rsqrt(jnp.mean(v * v, axis=-1, keepdims=True) + epsilon)
        return v * inverse * gain.astype(F32)

    scale = HEAD_DIM ** (-0.5) * math.log2(math.e)

    def project_queries(layer):
        normed = rms(stream[...].astype(F32), target_gains[layer, 0:1]).astype(BF16)
        queries[...] = (dot(normed, wq[layer]) * scale).astype(BF16)
        maxima[...] = jnp.full(maxima.shape, -1e30, F32)
        acc[...] = jnp.zeros(acc.shape, F32)

    def project_source(layer, j):
        normed = rms(
            src[j].reshape(chunk, src.shape[-1]).astype(F32), source_gain[layer : layer + 1]
        ).astype(BF16)
        keys[layer, j] = dot(normed, wk[layer]).astype(BF16)
        values[layer, j] = dot(normed, wv[layer]).astype(BF16)

    def attend(layer, j):
        for h in range(heads):
            cols = slice(h * HEAD_DIM, (h + 1) * HEAD_DIM)
            scores = lax.dot_general(
                queries[:, cols],
                keys[layer, j, :, cols],
                (((1,), (1,)), ((), ())),
                preferred_element_type=F32,
            )
            old = maxima[h]
            new = jnp.maximum(old, jnp.max(scores, axis=-1, keepdims=True))
            maxima[h] = new
            shrink = jnp.exp2(old - new)
            weights = jnp.exp2(scores - jnp.concatenate([new] * (chunk // HEAD_DIM), axis=1))
            block = values[layer, j, :, cols]
            block = jnp.concatenate([block, jnp.ones(block.shape, BF16)], axis=1)
            acc[h] = acc[h] * jnp.concatenate([shrink, shrink], axis=1) + dot(
                weights.astype(BF16), block
            )

    z_arrived(1, True)
    xcopy(0, stream.at[other_rows], stream.at[other_rows]).wait_recv()
    fetch[2, 0].wait()
    project_queries(0)
    xy_arrived(0)
    for k in (0, 1):
        for layer in range(layers):
            fetch[k, layer].wait()

    def plane(j, unused):
        @pl.when(j + 2 < size_z)
        def _():
            z_arrived(j + 2, False)

        @pl.when(j + 1 < size_z)
        def _():
            xy_arrived(j + 1)

        diag_arrived(j)

        @pl.when(j > 0)
        def _():
            to_tp(TZ, j, other).wait_recv()

        for kind in (TX, TY, TDX, TDY):
            to_tp(kind, j, other).wait_recv()
        for layer in range(layers):
            project_source(layer, j)
        attend(0, j)
        return unused

    lax.fori_loop(0, size_z, plane, 0)

    def exchanged(e, rows_of):
        return (
            part[e, rows_of].astype(F32) + got[e, rows_of].astype(F32)
        ).astype(BF16).astype(F32)

    give.wait_send()
    pending = []
    exchange = 0
    for layer in range(layers):
        if layer > 0:
            fetch[2, layer].wait()
            project_queries(layer)

            def again(j, unused, layer=layer):
                attend(layer, j)
                return unused

            lax.fori_loop(0, size_z, again, 0)
        fetch[3, layer].wait()
        e = exchange
        exchange += 1
        copies = []
        for b in range(2):
            sl = slice(b * own, (b + 1) * own)
            context = jnp.concatenate(
                [
                    (acc[h, sl, :HEAD_DIM] / acc[h, sl, HEAD_DIM:]).astype(BF16)
                    for h in range(heads)
                ],
                axis=1,
            )
            part[e, sl] = dot(context, wo[layer]).astype(BF16)
            c = xcopy(1 + 2 * e + b, part.at[e, sl], got.at[e, sl])
            c.start()
            copies.append(c)
        for k in (4, 5, 6):
            fetch[k, layer].wait()
        for b in range(2):
            sl = slice(b * own, (b + 1) * own)
            copies[b].wait_recv()
            stream[sl] = (
                stream[sl].astype(F32) + rms(exchanged(e, sl), target_gains[layer, 1:2])
            ).astype(BF16)
        pending += copies
        mixer_in = rms(stream[...].astype(F32), target_gains[layer, 2:3]).astype(BF16)
        gate = dot(mixer_in, wg[layer])
        hidden = (gate / (1.0 + jnp.exp(-gate)) * dot(mixer_in, wu[layer])).astype(BF16)
        e = exchange
        exchange += 1
        part[e] = dot(hidden, wd[layer]).astype(BF16)
        if layer < layers - 1:
            copies = []
            for b in range(2):
                sl = slice(b * own, (b + 1) * own)
                c = xcopy(1 + 2 * e + b, part.at[e, sl], got.at[e, sl])
                c.start()
                copies.append(c)
            for b in range(2):
                sl = slice(b * own, (b + 1) * own)
                copies[b].wait_recv()
                stream[sl] = (
                    stream[sl].astype(F32) + rms(exchanged(e, sl), target_gains[layer, 3:4])
                ).astype(BF16)
            pending += copies
        else:
            c = xcopy(1 + 2 * e, part.at[e, other_rows], got.at[e, other_rows])
            c.start()
            xcopy(1 + 2 * e, part.at[e, own_rows], got.at[e, own_rows]).wait_recv()
            out_ref[...] = (
                stream[own_rows].astype(F32)
                + rms(exchanged(e, own_rows), target_gains[layer, 3:4])
            ).astype(BF16)
            pending.append(c)
    for c in pending:
        c.wait_send()
    for j in range(size_z):
        if j > 0:
            to_z(j).wait_send()
            to_tp(TZ, j, core).wait_send()
        to_x(j).wait_send()
        to_y(j).wait_send()
        diag_x(j).wait_send()
        diag_y(j).wait_send()
        for kind in (TX, TY, TDX, TDY):
            to_tp(kind, j, core).wait_send()


def fused(grid, *args):
    target, source, target_gains, source_gain, wq, wk, wv, wo, wg, wu, wd = args
    layers, width, columns = wq.shape
    own, rows = target.shape[0], source.shape[0]
    heads = columns // HEAD_DIM
    size_z = grid[2]
    any_spec = pl.BlockSpec(memory_space=pl.ANY)
    vmem_spec = pl.BlockSpec(memory_space=pltpu.VMEM)
    return pl.pallas_call(
        functools.partial(fused_kernel, grid),
        out_shape=jax.ShapeDtypeStruct(target.shape, BF16),
        in_specs=[any_spec, any_spec, vmem_spec, vmem_spec] + [any_spec] * 7,
        out_specs=vmem_spec,
        scratch_shapes=[
            pltpu.VMEM((2 * own, width), BF16),
            pltpu.VMEM((size_z, 4, rows, width), BF16),
            *[pltpu.VMEM(w.shape, BF16) for w in (wq, wk, wv, wo, wg, wu, wd)],
            pltpu.VMEM((layers, size_z, 4 * rows, columns), BF16),
            pltpu.VMEM((layers, size_z, 4 * rows, columns), BF16),
            pltpu.VMEM((2 * own, columns), BF16),
            pltpu.VMEM((heads, 2 * own, HEAD_DIM), F32),
            pltpu.VMEM((heads, 2 * own, 2 * HEAD_DIM), F32),
            pltpu.VMEM((2 * layers, 2 * own, width), BF16),
            pltpu.VMEM((2 * layers, 2 * own, width), BF16),
            pltpu.SemaphoreType.DMA((10, size_z)),
            pltpu.SemaphoreType.DMA((10, size_z)),
            pltpu.SemaphoreType.DMA((1 + 4 * layers,)),
            pltpu.SemaphoreType.DMA((1 + 4 * layers,)),
            pltpu.SemaphoreType.DMA((7, layers)),
            pltpu.SemaphoreType.DMA((2,)),
        ],
        compiler_params=pltpu.CompilerParams(
            collective_id=0, has_side_effects=True, vmem_limit_bytes=60 * 1024 * 1024
        ),
    )(*args)


def chip_grid(mesh):
    devices = mesh.devices
    if mesh.axis_names != ("sp", "tp") or devices.shape[1] != 2:
        return None
    places = [tuple(d.coords) for d in devices[:, 0]]
    if [tuple(d.coords) for d in devices[:, 1]] != places:
        return None
    grid = tuple(max(p[k] for p in places) + 1 for k in range(3))
    expected = [
        (x, y, z) for z in range(grid[2]) for y in range(grid[1]) for x in range(grid[0])
    ]
    if places != expected or grid != (2, 2, 4):
        return None
    return grid


def solution(mesh):
    placed = (
        P(("sp", "tp"), None),
        P("sp", None),
        P(),
        P(),
        P(None, None, "tp"),
        P(None, None, "tp"),
        P(None, None, "tp"),
        P(None, "tp", None),
        P(None, None, "tp"),
        P(None, None, "tp"),
        P(None, "tp", None),
    )
    grid = chip_grid(mesh)
    body = per_device if grid is None else functools.partial(fused, grid)
    return jax.shard_map(
        body, mesh=mesh, in_specs=placed, out_specs=P(("sp", "tp"), None), check_vma=False
    )
```

```python
import functools
import math

import jax
import jax.numpy as jnp
from jax import lax
from jax.experimental import pallas as pl
from jax.experimental.pallas import tpu as pltpu
from jax.sharding import PartitionSpec as P

HEAD_DIM = 128


epsilon = 1e-06


def rms_norm(values, gain_row):
    widened = values.astype(jnp.float32)
    inverse = lax.rsqrt(jnp.mean(widened * widened, axis=-1, keepdims=True) + epsilon)
    return widened * inverse * gain_row.astype(jnp.float32)


def per_device(
    target,
    source,
    target_gains,
    source_gain,
    query_weight,
    key_weight,
    value_weight,
    out_weight,
    gate_weight,
    up_weight,
    down_weight,
):
    layers = query_weight.shape[0]
    own_rows = target.shape[0]
    heads_dev = query_weight.shape[2] // HEAD_DIM
    factor = HEAD_DIM ** (-0.5)

    def source_heads(layer_index):
        normed_source = rms_norm(source, source_gain[layer_index]).astype(jnp.bfloat16)
        key_rows = jnp.dot(
            normed_source, key_weight[layer_index], preferred_element_type=jnp.float32
        ).astype(jnp.bfloat16)
        value_rows = jnp.dot(
            normed_source, value_weight[layer_index], preferred_element_type=jnp.float32
        ).astype(jnp.bfloat16)
        return (key_rows, value_rows)

    projected = [source_heads(layer_index) for layer_index in range(layers)]
    every_key = jnp.stack([entry[0] for entry in projected])
    every_value = jnp.stack([entry[1] for entry in projected])
    every_key, every_value = (
        lax.all_gather(every_key, "sp", axis=1, tiled=True),
        lax.all_gather(every_value, "sp", axis=1, tiled=True),
    )
    sp_count = lax.axis_size("sp")
    source_rows = source.shape[0]
    grouping = 1
    while grouping * 2 * source_rows <= 512 and sp_count % (grouping * 2) == 0:
        grouping = grouping * 2
    stream = target
    for layer_index in range(layers):
        layer_gains = target_gains[layer_index]
        normed = rms_norm(stream, layer_gains[0]).astype(jnp.bfloat16)

        def query_piece(row_piece, offset, layer_index=layer_index):
            return jnp.dot(
                row_piece, query_weight[layer_index], preferred_element_type=jnp.float32
            ).astype(jnp.bfloat16)

        queries = query_piece(lax.all_gather(normed, "tp", axis=0, tiled=True), jnp.int32(0))
        group_rows = queries.shape[0]
        query_heads = queries.reshape(group_rows, heads_dev, HEAD_DIM)

        def attend(folded, pieces, offset, query_heads=query_heads):
            running_max, running_sum, weighted = folded
            key_heads = pieces[0].reshape(pieces[0].shape[0], heads_dev, HEAD_DIM)
            value_heads = pieces[1].reshape(pieces[1].shape[0], heads_dev, HEAD_DIM)
            scores = (
                jnp.einsum(
                    "thd,shd->ths", query_heads, key_heads, preferred_element_type=jnp.float32
                )
                * factor
            )
            new_max = jnp.maximum(running_max, jnp.max(scores, axis=-1))
            shrink = jnp.exp(running_max - new_max)
            weights = jnp.exp(scores - new_max[..., None])
            running_sum = running_sum * shrink + jnp.sum(weights, axis=-1)
            weighted = weighted * shrink[..., None] + jnp.einsum(
                "ths,shd->thd",
                weights.astype(jnp.bfloat16),
                value_heads,
                preferred_element_type=jnp.float32,
            )
            return (new_max, running_sum, weighted)

        initial = (
            jnp.full((group_rows, heads_dev), -1e30, jnp.float32),
            jnp.zeros((group_rows, heads_dev), jnp.float32),
            jnp.zeros((group_rows, heads_dev, HEAD_DIM), jnp.float32),
        )
        columns = every_key.shape[2]
        key_blocks = every_key[layer_index].reshape(
            sp_count // grouping, grouping * source_rows, columns
        )
        value_blocks = every_value[layer_index].reshape(
            sp_count // grouping, grouping * source_rows, columns
        )

        def scan_step(carry, blocks, attend=attend):
            return (attend(carry, blocks, 0), None)

        folded, unused = lax.scan(scan_step, initial, (key_blocks, value_blocks))
        running_max, running_sum, weighted = folded
        context = (
            (weighted / running_sum[..., None])
            .reshape(group_rows, heads_dev * HEAD_DIM)
            .astype(jnp.bfloat16)
        )

        def attn_term(offset, length, layer_index=layer_index, context=context):
            return jnp.dot(context, out_weight[layer_index], preferred_element_type=jnp.float32)

        attended = lax.psum_scatter(
            attn_term(jnp.int32(0), lax.axis_size("tp") * own_rows).astype(jnp.bfloat16),
            "tp",
            scatter_dimension=0,
            tiled=True,
        )
        stream = (stream.astype(jnp.float32) + rms_norm(attended, layer_gains[1])).astype(
            jnp.bfloat16
        )
        mixer_in = rms_norm(stream, layer_gains[2]).astype(jnp.bfloat16)

        def mixer_piece(row_piece, offset, layer_index=layer_index):
            gate_part = jnp.dot(
                row_piece, gate_weight[layer_index], preferred_element_type=jnp.float32
            )
            up_part = jnp.dot(row_piece, up_weight[layer_index], preferred_element_type=jnp.float32)
            return (jax.nn.silu(gate_part) * up_part).astype(jnp.bfloat16)

        hidden = mixer_piece(lax.all_gather(mixer_in, "tp", axis=0, tiled=True), jnp.int32(0))

        def mixer_term(offset, length, layer_index=layer_index, hidden=hidden):
            return jnp.dot(hidden, down_weight[layer_index], preferred_element_type=jnp.float32)

        mixer_out = lax.psum_scatter(
            mixer_term(jnp.int32(0), lax.axis_size("tp") * own_rows).astype(jnp.bfloat16),
            "tp",
            scatter_dimension=0,
            tiled=True,
        )
        stream = (stream.astype(jnp.float32) + rms_norm(mixer_out, layer_gains[3])).astype(
            jnp.bfloat16
        )
    return stream


MESH = pl.DeviceIdType.MESH
F32 = jnp.float32
BF16 = jnp.bfloat16
KZ, KX, KY, KDX, KDY, TZ, TX, TY, TDX, TDY = range(10)


def dot(a, b):
    return jnp.dot(a, b, preferred_element_type=F32)


def fused_kernel(
    grid,
    target,
    source,
    target_gains,
    source_gain,
    wq_hbm,
    wk_hbm,
    wv_hbm,
    wo_hbm,
    wg_hbm,
    wu_hbm,
    wd_hbm,
    out_ref,
    stream,
    src,
    wq,
    wk,
    wv,
    wo,
    wg,
    wu,
    wd,
    keys,
    values,
    queries,
    maxima,
    acc,
    part,
    got,
    send,
    recv,
    xsend,
    xrecv,
    wsem,
    lsem,
):
    size_x, size_y, size_z = grid
    layers = wq.shape[0]
    own = target.shape[0]
    rows = source.shape[0]
    heads = wq.shape[2] // HEAD_DIM
    half, quarter = rows // 2, rows // 4
    chunk = 4 * rows
    sp = lax.axis_index("sp")
    core = lax.axis_index("tp")
    other = 1 - core
    x = lax.rem(sp, size_x)
    y = lax.rem(lax.div(sp, size_x), size_y)
    z = lax.div(sp, size_x * size_y)

    def at(xx, yy, zz, cc):
        return {"sp": (zz * size_y + yy) * size_x + xx, "tp": cc}

    def flip(j):
        low = lax.rem(z + j, 2)
        high = lax.rem(lax.div(z, 2) + lax.div(j, 2), 2)
        return low + 2 * high

    x_peer = at(1 - x, y, z, core)
    y_peer = at(x, 1 - y, z, core)
    tp_peer = at(x, y, z, other)
    inner = lax.rem(lax.rem(z, 2) + lax.div(z, 2), 2)
    order = [jnp.int32(0), jnp.int32(1), 2 + inner, 3 - inner]

    own_rows = pl.ds(pl.multiple_of(core * own, own), own)
    other_rows = pl.ds(pl.multiple_of(other * own, own), own)
    source_copy = pltpu.make_async_copy(source, src.at[0, 0], lsem.at[0])
    target_copy = pltpu.make_async_copy(target, stream.at[own_rows], lsem.at[1])
    source_copy.start()
    target_copy.start()
    pairs = [(wk_hbm, wk), (wv_hbm, wv), (wq_hbm, wq), (wo_hbm, wo), (wg_hbm, wg), (wu_hbm, wu), (wd_hbm, wd)]
    fetch = {}
    for layer in range(layers):
        for k, (a, b) in enumerate(pairs):
            fetch[k, layer] = pltpu.make_async_copy(a.at[layer], b.at[layer], wsem.at[k, layer])

    barrier = pltpu.get_barrier_semaphore()
    peers = [x_peer, y_peer, tp_peer] + [at(x, y, flip(j), core) for j in order[1:]]
    for peer in peers:
        pl.semaphore_signal(barrier, inc=1, device_id=peer, device_id_type=MESH)
    for k in (2, 0, 1):
        fetch[k, 0].start()
    for k in (0, 1):
        for layer in range(1, layers):
            fetch[k, layer].start()
    pl.semaphore_wait(barrier, len(peers))

    def mine(c):
        return pl.ds(pl.multiple_of(c * half, half), half)

    def first(c):
        return pl.ds(pl.multiple_of(c * half, quarter), quarter)

    def second(c):
        return pl.ds(pl.multiple_of(c * half + quarter, quarter), quarter)

    def copy(kind, j, from_ref, to_ref, peer):
        return pltpu.make_async_remote_copy(
            src_ref=from_ref,
            dst_ref=to_ref,
            send_sem=send.at[kind, j],
            recv_sem=recv.at[kind, j],
            device_id=peer,
            device_id_type=MESH,
        )

    def blk(j, sub, sl):
        return src.at[j, sub, sl]

    def to_z(j):
        return copy(KZ, j, blk(0, 0, mine(core)), blk(j, 0, mine(core)), at(x, y, flip(j), core))

    def to_x(j):
        return copy(KX, j, blk(j, 0, mine(core)), blk(j, 1, mine(core)), x_peer)

    def to_y(j):
        return copy(KY, j, blk(j, 0, mine(core)), blk(j, 2, mine(core)), y_peer)

    def diag_y(j):
        return copy(KDY, j, blk(j, 1, first(core)), blk(j, 3, first(core)), y_peer)

    def diag_x(j):
        return copy(KDX, j, blk(j, 2, second(core)), blk(j, 3, second(core)), x_peer)

    def to_tp(kind, j, c):
        sub = {TZ: 0, TX: 1, TY: 2, TDX: 3, TDY: 3}[kind]
        sl = {TDX: second, TDY: first}.get(kind, mine)(c)
        return copy(kind, j, blk(j, sub, sl), blk(j, sub, sl), tp_peer)

    def z_arrived(zj):
        copy(KZ, zj, blk(zj, 0, mine(core)), blk(zj, 0, mine(core)), x_peer).wait_recv()
        to_x(zj).start()
        to_y(zj).start()
        to_tp(TZ, zj, core).start()

    def xy_arrived(j):
        copy(KX, j, blk(j, 1, mine(core)), blk(j, 1, mine(core)), x_peer).wait_recv()
        diag_y(j).start()
        to_tp(TX, j, core).start()
        copy(KY, j, blk(j, 2, mine(core)), blk(j, 2, mine(core)), y_peer).wait_recv()
        diag_x(j).start()
        to_tp(TY, j, core).start()

    def diag_arrived(j):
        copy(KDY, j, blk(j, 3, first(core)), blk(j, 3, first(core)), y_peer).wait_recv()
        to_tp(TDY, j, core).start()
        copy(KDX, j, blk(j, 3, second(core)), blk(j, 3, second(core)), x_peer).wait_recv()
        to_tp(TDX, j, core).start()

    def xcopy(e, from_ref, to_ref):
        return pltpu.make_async_remote_copy(
            src_ref=from_ref,
            dst_ref=to_ref,
            send_sem=xsend.at[e],
            recv_sem=xrecv.at[e],
            device_id=tp_peer,
            device_id_type=MESH,
        )

    source_copy.wait()
    to_x(0).start()
    to_y(0).start()
    for j in order[1:]:
        to_z(j).start()
    target_copy.wait()
    give = xcopy(0, stream.at[own_rows], stream.at[own_rows])
    give.start()
    for layer in range(layers):
        for k in (2, 3, 4, 5, 6):
            if (k, layer) != (2, 0):
                fetch[k, layer].start()

    def rms(v, gain):
        inverse = lax.rsqrt(jnp.mean(v * v, axis=-1, keepdims=True) + epsilon)
        return v * inverse * gain.astype(F32)

    scale = HEAD_DIM ** (-0.5) * math.log2(math.e)

    def project_queries(layer):
        normed = rms(stream[...].astype(F32), target_gains[layer, 0:1]).astype(BF16)
        queries[...] = (dot(normed, wq[layer]) * scale).astype(BF16)
        maxima[...] = jnp.full(maxima.shape, -1e30, F32)
        acc[...] = jnp.zeros(acc.shape, F32)

    def project_source(layer, j):
        normed = rms(
            src[j].reshape(chunk, src.shape[-1]).astype(F32), source_gain[layer : layer + 1]
        ).astype(BF16)
        keys[layer, j] = dot(normed, wk[layer]).astype(BF16)
        values[layer, j] = dot(normed, wv[layer]).astype(BF16)

    def attend(layer, j):
        for h in range(heads):
            cols = slice(h * HEAD_DIM, (h + 1) * HEAD_DIM)
            scores = lax.dot_general(
                queries[:, cols],
                keys[layer, j, :, cols],
                (((1,), (1,)), ((), ())),
                preferred_element_type=F32,
            )
            old = maxima[h]
            new = jnp.maximum(old, jnp.max(scores, axis=-1, keepdims=True))
            maxima[h] = new
            shrink = jnp.exp2(old - new)
            weights = jnp.exp2(scores - jnp.concatenate([new] * (chunk // HEAD_DIM), axis=1))
            block = values[layer, j, :, cols]
            block = jnp.concatenate([block, jnp.ones(block.shape, BF16)], axis=1)
            acc[h] = acc[h] * jnp.concatenate([shrink, shrink], axis=1) + dot(
                weights.astype(BF16), block
            )

    def complete(j, step):
        if step > 0:
            to_tp(TZ, j, other).wait_recv()
        for kind in (TX, TY, TDX, TDY):
            to_tp(kind, j, other).wait_recv()

    z_arrived(order[1])
    xcopy(0, stream.at[other_rows], stream.at[other_rows]).wait_recv()
    fetch[2, 0].wait()
    project_queries(0)
    xy_arrived(order[0])
    for k in (0, 1):
        for layer in range(layers):
            fetch[k, layer].wait()
    late = range(1, layers)
    xy_arrived(order[1])
    diag_arrived(order[0])
    complete(order[0], 0)
    project_source(0, order[0])
    z_arrived(order[2])
    for layer in late:
        project_source(layer, order[0])
    attend(0, order[0])
    z_arrived(order[3])
    diag_arrived(order[1])
    complete(order[1], 1)
    project_source(0, order[1])
    xy_arrived(order[2])
    for layer in late:
        project_source(layer, order[1])
    attend(0, order[1])
    xy_arrived(order[3])
    diag_arrived(order[2])
    complete(order[2], 2)
    project_source(0, order[2])
    for layer in late:
        project_source(layer, order[2])
    diag_arrived(order[3])
    attend(0, order[2])
    complete(order[3], 3)
    project_source(0, order[3])
    attend(0, order[3])

    give.wait_send()

    def exchanged(e, rows_of):
        return (
            part[e, rows_of].astype(F32) + got[e, rows_of].astype(F32)
        ).astype(BF16).astype(F32)

    pending = []
    exchange = 0
    for layer in range(layers):
        if layer > 0:
            fetch[2, layer].wait()
            project_queries(layer)

            def again(j, unused, layer=layer):
                attend(layer, j)
                return unused

            lax.fori_loop(0, size_z, again, 0)
        fetch[3, layer].wait()
        e = exchange
        exchange += 1
        copies = []
        for b in range(2):
            sl = slice(b * own, (b + 1) * own)
            context = jnp.concatenate(
                [
                    (acc[h, sl, :HEAD_DIM] / acc[h, sl, HEAD_DIM:]).astype(BF16)
                    for h in range(heads)
                ],
                axis=1,
            )
            part[e, sl] = dot(context, wo[layer]).astype(BF16)
            c = xcopy(1 + 2 * e + b, part.at[e, sl], got.at[e, sl])
            c.start()
            copies.append(c)
        for k in (4, 5, 6):
            fetch[k, layer].wait()
        if layer == 0:
            for k in late:
                project_source(k, order[3])
        for b in range(2):
            sl = slice(b * own, (b + 1) * own)
            copies[b].wait_recv()
            stream[sl] = (
                stream[sl].astype(F32) + rms(exchanged(e, sl), target_gains[layer, 1:2])
            ).astype(BF16)
        pending += copies
        mixer_in = rms(stream[...].astype(F32), target_gains[layer, 2:3]).astype(BF16)
        gate = dot(mixer_in, wg[layer])
        hidden = (gate / (1.0 + jnp.exp(-gate)) * dot(mixer_in, wu[layer])).astype(BF16)
        e = exchange
        exchange += 1
        if layer < layers - 1:
            copies = []
            for b in range(2):
                sl = slice(b * own, (b + 1) * own)
                part[e, sl] = dot(hidden[sl], wd[layer]).astype(BF16)
                c = xcopy(1 + 2 * e + b, part.at[e, sl], got.at[e, sl])
                c.start()
                copies.append(c)
            for b in range(2):
                sl = slice(b * own, (b + 1) * own)
                copies[b].wait_recv()
                stream[sl] = (
                    stream[sl].astype(F32) + rms(exchanged(e, sl), target_gains[layer, 3:4])
                ).astype(BF16)
            pending += copies
        else:
            part[e] = dot(hidden, wd[layer]).astype(BF16)
            c = xcopy(1 + 2 * e, part.at[e, other_rows], got.at[e, other_rows])
            c.start()
            xcopy(1 + 2 * e, part.at[e, own_rows], got.at[e, own_rows]).wait_recv()
            out_ref[...] = (
                stream[own_rows].astype(F32)
                + rms(exchanged(e, own_rows), target_gains[layer, 3:4])
            ).astype(BF16)
            pending.append(c)
    for c in pending:
        c.wait_send()
    for step, j in enumerate(order):
        if step > 0:
            to_z(j).wait_send()
            to_tp(TZ, j, core).wait_send()
        to_x(j).wait_send()
        to_y(j).wait_send()
        diag_x(j).wait_send()
        diag_y(j).wait_send()
        for kind in (TX, TY, TDX, TDY):
            to_tp(kind, j, core).wait_send()


def fused(grid, *args):
    target, source, target_gains, source_gain, wq, wk, wv, wo, wg, wu, wd = args
    layers, width, columns = wq.shape
    own, rows = target.shape[0], source.shape[0]
    heads = columns // HEAD_DIM
    size_z = grid[2]
    any_spec = pl.BlockSpec(memory_space=pl.ANY)
    vmem_spec = pl.BlockSpec(memory_space=pltpu.VMEM)
    return pl.pallas_call(
        functools.partial(fused_kernel, grid),
        out_shape=jax.ShapeDtypeStruct(target.shape, BF16),
        in_specs=[any_spec, any_spec, vmem_spec, vmem_spec] + [any_spec] * 7,
        out_specs=vmem_spec,
        scratch_shapes=[
            pltpu.VMEM((2 * own, width), BF16),
            pltpu.VMEM((size_z, 4, rows, width), BF16),
            *[pltpu.VMEM(w.shape, BF16) for w in (wq, wk, wv, wo, wg, wu, wd)],
            pltpu.VMEM((layers, size_z, 4 * rows, columns), BF16),
            pltpu.VMEM((layers, size_z, 4 * rows, columns), BF16),
            pltpu.VMEM((2 * own, columns), BF16),
            pltpu.VMEM((heads, 2 * own, HEAD_DIM), F32),
            pltpu.VMEM((heads, 2 * own, 2 * HEAD_DIM), F32),
            pltpu.VMEM((2 * layers, 2 * own, width), BF16),
            pltpu.VMEM((2 * layers, 2 * own, width), BF16),
            pltpu.SemaphoreType.DMA((10, size_z)),
            pltpu.SemaphoreType.DMA((10, size_z)),
            pltpu.SemaphoreType.DMA((1 + 4 * layers,)),
            pltpu.SemaphoreType.DMA((1 + 4 * layers,)),
            pltpu.SemaphoreType.DMA((7, layers)),
            pltpu.SemaphoreType.DMA((2,)),
        ],
        compiler_params=pltpu.CompilerParams(
            collective_id=0, has_side_effects=True, vmem_limit_bytes=60 * 1024 * 1024
        ),
    )(*args)


def chip_grid(mesh):
    devices = mesh.devices
    if mesh.axis_names != ("sp", "tp") or devices.shape[1] != 2:
        return None
    places = [tuple(d.coords) for d in devices[:, 0]]
    if [tuple(d.coords) for d in devices[:, 1]] != places:
        return None
    grid = tuple(max(p[k] for p in places) + 1 for k in range(3))
    expected = [
        (x, y, z) for z in range(grid[2]) for y in range(grid[1]) for x in range(grid[0])
    ]
    if places != expected or grid != (2, 2, 4):
        return None
    return grid


def solution(mesh):
    placed = (
        P(("sp", "tp"), None),
        P("sp", None),
        P(),
        P(),
        P(None, None, "tp"),
        P(None, None, "tp"),
        P(None, None, "tp"),
        P(None, "tp", None),
        P(None, None, "tp"),
        P(None, None, "tp"),
        P(None, "tp", None),
    )
    grid = chip_grid(mesh)
    body = per_device if grid is None else functools.partial(fused, grid)
    return jax.shard_map(
        body, mesh=mesh, in_specs=placed, out_specs=P(("sp", "tp"), None), check_vma=False
    )
```
